32 devices in a mesh: kv: 8 (over z, y), tp: 4 (over x, core).
Axes of the slice: x: 2, y: 2, z: 4, core: 2. Of those that a mesh axis runs over, the one named last changes fastest.
Arguments:
- tokens: bfloat16 [32, 4096], P(None, 'kv'), may hold values from -40 to 40, as said below
- norm_gain: float32 [4096], P('kv'), may hold values from 0.1 to 1.9
- w_query: bfloat16 [4096, 2048], P('kv', 'tp'), may hold values from -0.09375 to 0.09375
- w_key: bfloat16 [4096, 512], P('kv', 'tp'), may hold values from -0.09375 to 0.09375
- w_value: bfloat16 [4096, 512], P('kv', 'tp'), may hold values from -0.09375 to 0.09375
- forget_weight: bfloat16 [4096, 32], replicated, may hold values from -0.09375 to 0.09375
- forget_bias: float32 [32], P('tp'), may hold values from -1 to 3
- kv_cache: bfloat16 [32, 10240, 8, 128], P(None, 'kv', 'tp'), may hold values from -6 to 6
- cum_gates: float32 [32, 32, 10240], P(None, 'tp', 'kv'), may hold values from -10500 to 0, as said below
- lengths: int32 [32], replicated, may hold values from 1 to 10240, as said below
- w_out: bfloat16 [2048, 4096], P('tp', 'kv'), may hold values from -0.25 to 0.25
Outputs:
- mixed: bfloat16 [32, 4096], P(None, 'kv')
- log_weight: float32 [32, 32], P(None, 'tp')
The draws below stay inside these ranges and needn't reach their ends.
Inputs may be any that keep to these rules, and one draw needn't show every extreme that they name: Columns of tokens come in 16 groups of equal width. `cum_gates`: each row does not rise along the positions. `lengths`: some sequence has all 10240 positions cached.
All inputs are finite; a program needn't handle non-finite values.
Results may differ from the reference program's by a relative error of at most 0.0307.
Values may be sent and summed in bfloat16 or wider, within the bound.
No kernel may reach another device: no remote copies, remote signals or barrier semaphores. Data moves between devices by JAX's collectives and lax.ppermute only.
A program may use at most 128 MiB of HBM per device.

```python
import math
import jax
import jax.numpy as jnp
from jax import lax

D = 4096
HEADS = 32
KV_HEADS = 8
HEAD = 64
BATCH = 32
CTX_DEV = 1280
LENGTH = 10240
N_KV = 8
N_TP = 4


def draw_tokens(key, part):
    first_key, second_key, third_key = jax.random.split(key, 3)
    base = jax.random.normal(first_key, (BATCH, D), jnp.float32)
    group_scale = jnp.exp(jax.random.uniform(second_key, (16,), jnp.float32, math.log(0.3), math.log(3.0)))
    columns = jnp.repeat(group_scale, D // 16)
    values = base * columns
    return jnp.clip(values, -40.0, 40.0).astype(jnp.bfloat16)


def draw_cum_gates(key, part):
    first_key, second_key, third_key = jax.random.split(key, 3)
    shift_key = jax.random.fold_in(key, 11)
    pick_key, depth_key, forced_key = jax.random.split(shift_key, 3)
    fast_share = 0.5
    is_fast = jax.random.uniform(first_key, (BATCH, HEADS), jnp.float32) < fast_share
    rate = jnp.where(is_fast, 1.0 / 30.0, 1.0 / LENGTH)
    block_factor = jnp.exp(jax.random.uniform(second_key, (BATCH, HEADS, LENGTH // CTX_DEV), jnp.float32, math.log(0.35), math.log(2.8)))
    block_factor = jnp.repeat(block_factor, CTX_DEV, axis=2)
    step_size = jax.random.uniform(third_key, (BATCH, HEADS, LENGTH), jnp.float32, 0.2, 1.8)
    log_forget = -rate[:, :, None] * block_factor * step_size
    shifted = jax.random.uniform(pick_key, (BATCH, HEADS), jnp.float32) < 0.25
    depth = jax.random.uniform(depth_key, (BATCH, HEADS), jnp.float32, 120.0, 260.0)
    forced = jax.random.randint(forced_key, (), 0, BATCH * HEADS)
    flat_index = jnp.arange(BATCH * HEADS, dtype=jnp.int32).reshape(BATCH, HEADS)
    offset = jnp.where(shifted, -depth, 0.0)
    offset = jnp.where(flat_index == forced, -jnp.maximum(depth, 200.0), offset)
    return jnp.cumsum(log_forget, axis=2) + offset[:, :, None]


def draw_lengths(key, part):
    first_key, second_key = jax.random.split(key)
    values = jax.random.randint(first_key, (BATCH,), 1, LENGTH + 1).astype(jnp.int32)
    chosen = jax.random.randint(second_key, (), 0, BATCH)
    return values.at[chosen].set(LENGTH).astype(jnp.int32)


def level_of(key, shape, cuts, low, largest):
    gain = 1.0
    for axis_at, blocks in cuts:
        draws = jax.random.uniform(jax.random.fold_in(jax.random.fold_in(key, 6), axis_at), (blocks,), jnp.float32, low / len(cuts), largest / len(cuts))
        gain = gain * jnp.repeat(jnp.exp(draws), shape[axis_at] // blocks).reshape((-1,) + (1,) * (len(shape) - 1 - axis_at))
    return gain


def noise(rng, dims, scale, most, cuts=(), kind=jnp.bfloat16):
    entries = jax.random.normal(rng, dims, jnp.float32) * scale
    if len(cuts) > 0:
        entries = level_of(rng, dims, cuts, -0.22, 0.18) * entries
    return jnp.clip(entries, min=-most, max=most).astype(kind)


def setup_inputs(seed: int = 0) -> dict:
    key_list = jax.random.split(jax.random.key(seed), 12)
    tokens = draw_tokens(jax.random.fold_in(key_list[11], 71), 0)
    norm_gain = jnp.clip(1.0 + 0.18 * jax.random.normal(key_list[1], (D,), jnp.float32), 0.1, 1.9)
    w_query = noise(key_list[2], (D, HEADS * HEAD), D ** -0.5, 0.09375, ((0, 8), (1, 4)))
    w_key = noise(key_list[3], (D, KV_HEADS * HEAD), D ** -0.5, 0.09375, ((0, 8), (1, 4)))
    w_value = noise(key_list[4], (D, KV_HEADS * HEAD), D ** -0.5, 0.09375, ((0, 8), (1, 4)))
    forget_weight = noise(key_list[5], (D, HEADS), D ** -0.5, 0.09375)
    forget_bias = jnp.clip(-1.0 + 4.0 * jax.random.uniform(key_list[6], (HEADS,), jnp.float32) ** level_of(key_list[6], (HEADS,), ((0, 4),), -0.2, 0.2), -1.0, 3.0)
    kv_cache = noise(key_list[7], (BATCH, LENGTH, KV_HEADS, 2 * HEAD), 1.0, 6.0, ((1, 8), (2, 4)))
    cum_gates = draw_cum_gates(jax.random.fold_in(key_list[11], 71), 0)
    lengths = draw_lengths(jax.random.fold_in(key_list[11], 71), 0)
    w_out = noise(key_list[10], (HEADS * HEAD, D), (HEAD * 8) ** -0.5, 0.25, ((0, 4), (1, 8)))
    return dict(tokens=tokens, norm_gain=norm_gain, w_query=w_query, w_key=w_key, w_value=w_value, forget_weight=forget_weight, forget_bias=forget_bias, kv_cache=kv_cache, cum_gates=cum_gates, lengths=lengths, w_out=w_out)


norm_eps = 1e-05
masked_floor = -1e+30

def reference(tokens, norm_gain, w_query, w_key, w_value, forget_weight, forget_bias, kv_cache, cum_gates, lengths, w_out):
    tokens_f = tokens.astype(jnp.float32)
    row_scale = lax.rsqrt(lax.optimization_barrier(jnp.mean(tokens_f * tokens_f, axis=1)) + norm_eps)[:, None]
    normalized_input = (tokens_f * norm_gain).astype(jnp.bfloat16)
    query = (row_scale * jnp.dot(normalized_input, w_query, preferred_element_type=jnp.float32)).astype(jnp.bfloat16)
    fresh_key_row = (row_scale * jnp.dot(normalized_input, w_key, preferred_element_type=jnp.float32)).astype(jnp.bfloat16)
    value_new = (row_scale * jnp.dot(normalized_input, w_value, preferred_element_type=jnp.float32)).astype(jnp.bfloat16)
    log_gate = jax.nn.log_sigmoid(row_scale * jnp.dot(normalized_input, forget_weight, preferred_element_type=jnp.float32) + forget_bias)
    group_size = HEADS // KV_HEADS
    inv_root = HEAD ** (-0.5)

    def one_row(items):
        query_row, key_row, value_row, forget_gate_row, cache_row, cum_row, length = items
        query_head_rows = query_row.astype(jnp.float32).reshape(KV_HEADS, group_size, HEAD)
        cached_keys = cache_row[:, :, :HEAD].astype(jnp.float32)
        cached_vals = cache_row[:, :, HEAD:].astype(jnp.float32)
        scores = jnp.einsum('kgd,lkd->kgl', query_head_rows, cached_keys) * inv_root
        biased = scores - cum_row.reshape(KV_HEADS, group_size, LENGTH)
        last_cum = lax.dynamic_index_in_dim(cum_row, (length - 1).astype(jnp.int32), axis=1, keepdims=False)
        cum_query = last_cum + forget_gate_row
        key_heads = key_row.astype(jnp.float32).reshape(KV_HEADS, HEAD)
        new_biased = jnp.einsum('kgd,kd->kg', query_head_rows, key_heads) * inv_root - cum_query.reshape(KV_HEADS, group_size)
        blocked = biased.reshape(KV_HEADS, group_size, N_KV, CTX_DEV)
        in_range = (jnp.arange(LENGTH, dtype=jnp.int32) < length).reshape(N_KV, CTX_DEV)
        holds_last = jnp.arange(N_KV, dtype=jnp.int32) == (length - 1) // CTX_DEV
        block_peak = lax.optimization_barrier(jnp.max(jnp.where(in_range, blocked, masked_floor), axis=-1))
        block_peak = jnp.where(holds_last, jnp.maximum(block_peak, new_biased[..., None]), block_peak)
        weights = jnp.where(in_range, jnp.exp(blocked - block_peak[..., None]), 0.0)
        new_weight = jnp.where(holds_last, jnp.exp(new_biased[..., None] - block_peak), 0.0)
        block_sum = lax.optimization_barrier(jnp.sum(weights, axis=-1)) + new_weight
        rounded = lax.optimization_barrier(weights.astype(jnp.bfloat16)).astype(jnp.float32)
        rounded_new = lax.optimization_barrier(new_weight.astype(jnp.bfloat16)).astype(jnp.float32)
        value_block_rows = jnp.einsum('kgnl,nlkd->kgnd', rounded, cached_vals.reshape(N_KV, CTX_DEV, KV_HEADS, HEAD))
        value_heads = value_row.astype(jnp.float32).reshape(KV_HEADS, 1, 1, HEAD)
        value_block_rows = value_block_rows + rounded_new[..., None] * value_heads
        peak = lax.optimization_barrier(jnp.max(block_peak, axis=-1))
        rescale_factor = jnp.exp(block_peak - peak[..., None])
        weight_sum = lax.optimization_barrier(jnp.sum(block_sum * rescale_factor, axis=-1))
        values = lax.optimization_barrier(jnp.sum(value_block_rows * rescale_factor[..., None], axis=2))
        attended = (values / weight_sum[..., None]).astype(jnp.bfloat16).reshape(HEADS * HEAD)
        log_weight = (peak + jnp.log(weight_sum)).reshape(HEADS) + cum_query
        return (attended, log_weight)
    attended, log_weight = lax.map(one_row, (query, fresh_key_row, value_new, log_gate, kv_cache, cum_gates, lengths))
    group_cols = HEADS * HEAD // N_TP
    pieces = attended.astype(jnp.float32).reshape(BATCH, N_TP, group_cols)
    out_rows = w_out.astype(jnp.float32).reshape(N_TP, group_cols, D)
    partial_out = jnp.einsum('bgc,gcd->gbd', pieces, out_rows).astype(jnp.bfloat16)
    partial_out = lax.optimization_barrier(partial_out)
    mixed = lax.optimization_barrier(jnp.sum(partial_out.astype(jnp.float32), axis=0)).astype(jnp.bfloat16)
    return (mixed, log_weight)
```

```python
import functools

import jax
import jax.numpy as jnp
from jax import lax
from jax.experimental import pallas as pl
from jax.experimental.pallas import tpu as pltpu
from jax.sharding import PartitionSpec as P

norm_eps = 1e-05
masked_floor = -1e30
lanes = 128


def rounded(x):
    return x.astype(jnp.bfloat16).astype(jnp.float32)


def xor_permute(x, axis, step):
    size = lax.axis_size(axis)
    return lax.ppermute(x, axis, [(i, i ^ step) for i in range(size)])


def exchange_sum(x, axis):
    step = 1
    while step < lax.axis_size(axis):
        mine = lax.optimization_barrier(x.astype(jnp.bfloat16))
        other = xor_permute(mine, axis, step)
        x = mine.astype(jnp.float32) + other.astype(jnp.float32)
        step *= 2
    return x


def expand_body(rel_ref, cum_ref, bias_ref, last_ref, *, kv_local, group):
    rows, heads, span = cum_ref.shape
    wide = lanes * kv_local
    half = span * kv_local // 2
    spread = (
        lax.broadcasted_iota(jnp.int32, (lanes, wide), 1) // kv_local
        == lax.broadcasted_iota(jnp.int32, (lanes, wide), 0)
    ).astype(jnp.bfloat16)
    spread2 = jnp.concatenate([spread, spread], axis=0)
    col = lax.broadcasted_iota(jnp.int32, (heads, wide), 1)
    row_head = lax.broadcasted_iota(jnp.int32, (heads, wide), 0) // group
    own = col % kv_local == row_head
    local = col // kv_local
    narrow = lax.broadcasted_iota(jnp.int32, (heads, lanes), 1)
    base = pl.program_id(0) * rows
    last = [jnp.zeros((heads, lanes), jnp.float32) for _ in range(rows)]
    for c in range(span // lanes):
        x = cum_ref[:, :, c * lanes : (c + 1) * lanes].reshape(rows * heads, lanes)
        high = rounded(x)
        mid = rounded(x - high)
        low = (x - high - mid).astype(jnp.bfloat16)
        pair = jnp.concatenate([high.astype(jnp.bfloat16), mid.astype(jnp.bfloat16)], axis=1)
        y = jnp.dot(pair, spread2, preferred_element_type=jnp.float32) + jnp.dot(
            low, spread, preferred_element_type=jnp.float32
        )
        start = c * wide
        side = start // half
        start = start - side * half
        for r in range(rows):
            rel = rel_ref[base + r] - c * lanes
            ok = own & (local < rel)
            bias_ref[r, side * heads : (side + 1) * heads, start : start + wide] = jnp.where(
                ok, y[r * heads : (r + 1) * heads], -masked_floor
            )
            last[r] = last[r] + jnp.where(
                narrow == rel - 1, x[r * heads : (r + 1) * heads], 0.0
            )
    for r in range(rows):
        last_ref[r] = jnp.broadcast_to(jnp.sum(last[r], axis=1, keepdims=True), (heads, lanes))


def expand_gates(rel_len, cum_gates, kv_local, group):
    batch, heads, span = cum_gates.shape
    rows = 8
    half = span * kv_local // 2
    return pl.pallas_call(
        functools.partial(expand_body, kv_local=kv_local, group=group),
        grid_spec=pltpu.PrefetchScalarGridSpec(
            num_scalar_prefetch=1,
            grid=(batch // rows,),
            in_specs=[pl.BlockSpec((rows, heads, span), lambda i, rel: (i, 0, 0))],
            out_specs=[
                pl.BlockSpec((rows, 2 * heads, half), lambda i, rel: (i, 0, 0)),
                pl.BlockSpec((rows, heads, lanes), lambda i, rel: (i, 0, 0)),
            ],
        ),
        out_shape=[
            jax.ShapeDtypeStruct((batch, 2 * heads, half), jnp.float32),
            jax.ShapeDtypeStruct((batch, heads, lanes), jnp.float32),
        ],
        name="expand_gates",
    )(rel_len, cum_gates)


def attend_body(query_ref, cache_ref, bias_ref, out_ref, *, scale):
    rows, length, width = cache_ref.shape
    heads = query_ref.shape[1] // 2
    half = length // 2
    lane = lax.broadcasted_iota(jnp.int32, (heads, width), 1)
    for r in range(rows):
        both = jnp.concatenate([cache_ref[r, :half], cache_ref[r, half:]], axis=1)
        scores = lax.dot_general(
            query_ref[r], both, (((1,), (1,)), ((), ())), preferred_element_type=jnp.float32
        )
        biased = scores * scale - bias_ref[r]
        peak = jnp.max(biased, axis=1, keepdims=True)
        peak = jnp.maximum(jnp.maximum(peak[:heads], peak[heads:]), masked_floor)
        weights = jnp.exp(biased - jnp.concatenate([peak, peak], axis=0))
        total = jnp.sum(weights, axis=1, keepdims=True)
        total = total[:heads] + total[heads:]
        values = jnp.dot(weights.astype(jnp.bfloat16), both, preferred_element_type=jnp.float32)
        values = values[:heads, :width] + values[heads:, width:]
        out_ref[r] = jnp.where(lane == 0, peak, jnp.where(lane == 1, total, values))


def attend(query, cache, bias, scale):
    batch, length, width = cache.shape
    rows = 4
    heads = query.shape[1] // 2

    def spec(*shape):
        return pl.BlockSpec((rows,) + shape, lambda i: (i, 0, 0))

    return pl.pallas_call(
        functools.partial(attend_body, scale=scale),
        grid=(batch // rows,),
        in_specs=[
            spec(2 * heads, 2 * width),
            spec(length, width),
            spec(2 * heads, length // 2),
        ],
        out_specs=spec(heads, width),
        out_shape=jax.ShapeDtypeStruct((batch, heads, width), jnp.float32),
        name="attend",
    )(query, cache, bias)


def read_field(stats, index, heads):
    parts = [
        pltpu.roll(stats, (lanes - (3 * index + t) * heads) % lanes, 1) for t in range(3)
    ]
    return parts[0] + (parts[1] + parts[2])


def write_field(x, index, heads):
    high = rounded(x)
    mid = rounded(x - high)
    low = rounded(x - high - mid)
    out = 0.0
    for t, part in enumerate((high, mid, low)):
        out = out + pltpu.roll(part, (3 * index + t) * heads, 1)
    return out


def spread_factors(factors, heads, head_size):
    width = heads * head_size
    stacked = jnp.concatenate(factors, axis=0)
    high = rounded(stacked)
    pair = jnp.concatenate(
        [high.astype(jnp.bfloat16), (stacked - high).astype(jnp.bfloat16)], axis=1
    )
    spread = (
        lax.broadcasted_iota(jnp.int32, (2 * lanes, width), 1) // head_size
        == lax.broadcasted_iota(jnp.int32, (2 * lanes, width), 0) % lanes
    ).astype(jnp.bfloat16)
    wide = jnp.dot(pair, spread, preferred_element_type=jnp.float32)
    rows = factors[0].shape[0]
    return [wide[i * rows : (i + 1) * rows] for i in range(len(factors))]


def merge_stats(mine_ref, other_ref, heads, width):
    own_stats = mine_ref[:, width:].astype(jnp.float32)
    far_stats = other_ref[:, width:].astype(jnp.float32)
    used = lax.broadcasted_iota(jnp.int32, own_stats.shape, 1) < heads
    own_peak, far_peak = (read_field(s, 0, heads) for s in (own_stats, far_stats))
    own_sum, far_sum = (read_field(s, 1, heads) for s in (own_stats, far_stats))
    anchor = read_field(own_stats, 2, heads) + read_field(far_stats, 2, heads)
    own_peak, far_peak, anchor, own_sum, far_sum = (
        jnp.where(used, x, 0.0) for x in (own_peak, far_peak, anchor, own_sum, far_sum)
    )
    peak = jnp.maximum(own_peak, far_peak)
    own_factor = jnp.exp(own_peak - peak)
    far_factor = jnp.exp(far_peak - peak)
    total = own_sum * own_factor + far_sum * far_factor
    return used, peak, total, anchor, own_factor, far_factor


def merge_body(mine_ref, other_ref, out_ref, *, heads, head_size):
    width = heads * head_size
    used, peak, total, anchor, own_factor, far_factor = merge_stats(
        mine_ref, other_ref, heads, width
    )
    own_wide, far_wide = spread_factors(
        [jnp.where(used, own_factor, 0.0), jnp.where(used, far_factor, 0.0)], heads, head_size
    )
    values = own_wide * mine_ref[:, :width].astype(jnp.float32) + far_wide * other_ref[
        :, :width
    ].astype(jnp.float32)
    out_ref[:, :width] = values.astype(jnp.bfloat16)
    stats = (
        write_field(peak, 0, heads)
        + write_field(jnp.where(used, total, 0.0), 1, heads)
        + write_field(anchor, 2, heads)
    )
    out_ref[:, width:] = stats.astype(jnp.bfloat16)


def merge(mine, other, heads, head_size):
    return pl.pallas_call(
        functools.partial(merge_body, heads=heads, head_size=head_size),
        out_shape=jax.ShapeDtypeStruct(mine.shape, mine.dtype),
        name="merge",
    )(mine, other)


def finish_body(
    mine_ref, other_ref, fresh_ref, value_ref, attended_ref, log_ref, *, heads, head_size
):
    width = heads * head_size
    used, peak, total, anchor, own_factor, far_factor = merge_stats(
        mine_ref, other_ref, heads, width
    )
    fresh = fresh_ref[...]
    cum_query = anchor + pltpu.roll(fresh, lanes - heads, 1)
    fresh_biased = jnp.where(used, fresh - cum_query, 0.0)
    top = jnp.maximum(peak, fresh_biased)
    keep = jnp.exp(peak - top)
    fresh_weight = jnp.exp(fresh_biased - top)
    total = jnp.where(used, total * keep + fresh_weight, 1.0)
    factors = [own_factor * keep / total, far_factor * keep / total, rounded(fresh_weight) / total]
    own_wide, far_wide, fresh_wide = spread_factors(
        [jnp.where(used, f, 0.0) for f in factors], heads, head_size
    )
    values = (
        own_wide * mine_ref[:, :width].astype(jnp.float32)
        + far_wide * other_ref[:, :width].astype(jnp.float32)
        + fresh_wide * value_ref[...].astype(jnp.float32)
    )
    attended_ref[...] = values.astype(jnp.bfloat16)
    log_ref[...] = top + jnp.log(total) + cum_query


def finish(mine, other, fresh, value, heads, head_size):
    batch = mine.shape[0]
    return pl.pallas_call(
        functools.partial(finish_body, heads=heads, head_size=head_size),
        out_shape=[
            jax.ShapeDtypeStruct((batch, heads * head_size), jnp.bfloat16),
            jax.ShapeDtypeStruct((batch, lanes), jnp.float32),
        ],
        name="finish",
    )(mine, other, fresh, value)


def split_three(x):
    high = lax.reduce_precision(x, 8, 7)
    mid = lax.reduce_precision(x - high, 8, 7)
    low = lax.reduce_precision(x - high - mid, 8, 7)
    return [high, mid, low]


def shards(
    tokens,
    norm_gain,
    w_query,
    w_key,
    w_value,
    forget_weight,
    forget_bias,
    kv_cache,
    cum_gates,
    lengths,
    w_out,
):
    batch, cols = tokens.shape
    span = kv_cache.shape[1]
    kv_local = kv_cache.shape[2]
    head_size = kv_cache.shape[3] // 2
    heads = cum_gates.shape[1]
    group = heads // kv_local
    width = heads * head_size
    kv_width = kv_local * head_size
    model_width = cols * lax.axis_size("kv")

    first_pos = lax.axis_index("kv") * span
    bias, last_cum = expand_gates(lengths - first_pos, cum_gates, kv_local, group)

    tokens_f = tokens.astype(jnp.float32)
    squares = jnp.sum(tokens_f * tokens_f, axis=1, keepdims=True)
    normed = (tokens_f * norm_gain).astype(jnp.bfloat16)
    gate_cols = lax.dynamic_slice(
        forget_weight,
        (lax.axis_index("kv") * cols, lax.axis_index("tp") * heads),
        (cols, heads),
    )
    parts = [
        jnp.dot(normed, w, preferred_element_type=jnp.float32)
        for w in (w_query, w_key, w_value, gate_cols)
    ]
    parts.append(squares)
    used = sum(p.shape[1] for p in parts)
    parts.append(jnp.zeros((batch, -used % lanes), jnp.float32))
    sums = exchange_sum(jnp.concatenate(parts, axis=1), "kv")

    edge = width + 2 * kv_width
    row_scale = lax.rsqrt(sums[:, edge + heads : edge + heads + 1] / model_width + norm_eps)
    projected = (row_scale * sums[:, :edge]).astype(jnp.bfloat16)
    query = projected[:, :width]
    log_gate = jax.nn.log_sigmoid(row_scale * sums[:, edge : edge + heads] + forget_bias)
    query_rows = query.reshape(batch, heads, head_size)
    full = 4 * head_size
    query_pair = jnp.concatenate(
        [
            jnp.pad(query_rows, ((0, 0), (0, 0), (0, full - head_size))),
            jnp.pad(query_rows, ((0, 0), (0, 0), (full // 2, full // 2 - head_size))),
        ],
        axis=1,
    )
    scale = head_size ** (-0.5)
    cache = kv_cache.reshape(batch, span * kv_local, 2 * head_size)
    partial = attend(query_pair, cache, bias, scale)

    key_rows = projected[:, width : width + kv_width].reshape(batch, kv_local, 1, head_size)
    fresh_score = jnp.sum(
        query.reshape(batch, kv_local, group, head_size).astype(jnp.float32)
        * key_rows.astype(jnp.float32),
        axis=-1,
    ).reshape(batch, heads)
    fresh = jnp.concatenate(
        [
            fresh_score * scale,
            log_gate,
            jnp.zeros((batch, lanes - 2 * heads), jnp.float32),
        ],
        axis=1,
    )
    value_rows = projected[:, width + kv_width :].reshape(batch, kv_local, 1, head_size)
    value_wide = jnp.broadcast_to(value_rows, (batch, kv_local, group, head_size)).reshape(
        batch, width
    )

    stats = split_three(partial[:, :, 0]) + split_three(partial[:, :, 1])
    stats = stats + split_three(last_cum[:, :, 0])
    stats.append(jnp.zeros((batch, lanes - 9 * heads), jnp.float32))
    packed = jnp.concatenate(
        [partial[:, :, head_size:].reshape(batch, width)] + stats, axis=1
    ).astype(jnp.bfloat16)

    step = 1
    while 2 * step < lax.axis_size("kv"):
        packed = merge(packed, xor_permute(packed, "kv", step), heads, head_size)
        step *= 2
    attended, log_weight = finish(
        packed, xor_permute(packed, "kv", step), fresh, value_wide, heads, head_size
    )
    part_out = jnp.dot(attended, w_out, preferred_element_type=jnp.float32)
    mixed = exchange_sum(part_out, "tp").astype(jnp.bfloat16)
    return (mixed, log_weight[:, :heads])


def solution(mesh):
    placed = (
        P(None, "kv"),
        P("kv"),
        P("kv", "tp"),
        P("kv", "tp"),
        P("kv", "tp"),
        P(),
        P("tp"),
        P(None, "kv", "tp", None),
        P(None, "tp", "kv"),
        P(),
        P("tp", "kv"),
    )
    return jax.shard_map(
        shards,
        mesh=mesh,
        in_specs=placed,
        out_specs=(P(None, "kv"), P(None, "tp")),
        check_vma=False,
    )
```

```python
import functools

import jax
import jax.numpy as jnp
from jax import lax
from jax.experimental import pallas as pl
from jax.experimental.pallas import tpu as pltpu
from jax.sharding import PartitionSpec as P

norm_eps = 1e-05
masked_floor = -1e30
lanes = 128


def rounded(x):
    return x.astype(jnp.bfloat16).astype(jnp.float32)


def xor_permute(x, axis, step):
    size = lax.axis_size(axis)
    return lax.ppermute(x, axis, [(i, i ^ step) for i in range(size)])


def exchange_sum(x, axis):
    step = 1
    while step < lax.axis_size(axis):
        mine = lax.optimization_barrier(x.astype(jnp.bfloat16))
        other = xor_permute(mine, axis, step)
        x = mine.astype(jnp.float32) + other.astype(jnp.float32)
        step *= 2
    return x


def expand_body(rel_ref, cum_ref, bias_ref, last_ref, *, kv_local, group):
    rows, heads, span = cum_ref.shape
    wide = lanes * kv_local
    half = span * kv_local // 2
    spread = (
        lax.broadcasted_iota(jnp.int32, (lanes, wide), 1) // kv_local
        == lax.broadcasted_iota(jnp.int32, (lanes, wide), 0)
    ).astype(jnp.bfloat16)
    spread2 = jnp.concatenate([spread, spread], axis=0)
    col = lax.broadcasted_iota(jnp.int32, (heads, wide), 1)
    row_head = lax.broadcasted_iota(jnp.int32, (heads, wide), 0) // group
    own = col % kv_local == row_head
    local = col // kv_local
    narrow = lax.broadcasted_iota(jnp.int32, (heads, lanes), 1)
    base = pl.program_id(0) * rows
    last = [jnp.zeros((heads, lanes), jnp.float32) for _ in range(rows)]
    for c in range(span // lanes):
        x = cum_ref[:, :, c * lanes : (c + 1) * lanes].reshape(rows * heads, lanes)
        high = rounded(x)
        mid = rounded(x - high)
        low = (x - high - mid).astype(jnp.bfloat16)
        pair = jnp.concatenate([high.astype(jnp.bfloat16), mid.astype(jnp.bfloat16)], axis=1)
        y = jnp.dot(pair, spread2, preferred_element_type=jnp.float32) + jnp.dot(
            low, spread, preferred_element_type=jnp.float32
        )
        start = c * wide
        side = start // half
        start = start - side * half
        for r in range(rows):
            rel = rel_ref[base + r] - c * lanes
            ok = own & (local < rel)
            bias_ref[r, side * heads : (side + 1) * heads, start : start + wide] = jnp.where(
                ok, y[r * heads : (r + 1) * heads], -masked_floor
            )
            last[r] = last[r] + jnp.where(
                narrow == rel - 1, x[r * heads : (r + 1) * heads], 0.0
            )
    for r in range(rows):
        last_ref[r] = jnp.broadcast_to(jnp.sum(last[r], axis=1, keepdims=True), (heads, lanes))


def expand_gates(rel_len, cum_gates, kv_local, group):
    batch, heads, span = cum_gates.shape
    rows = 8
    half = span * kv_local // 2
    return pl.pallas_call(
        functools.partial(expand_body, kv_local=kv_local, group=group),
        grid_spec=pltpu.PrefetchScalarGridSpec(
            num_scalar_prefetch=1,
            grid=(batch // rows,),
            in_specs=[pl.BlockSpec((rows, heads, span), lambda i, rel: (i, 0, 0))],
            out_specs=[
                pl.BlockSpec((rows, 2 * heads, half), lambda i, rel: (i, 0, 0)),
                pl.BlockSpec((rows, heads, lanes), lambda i, rel: (i, 0, 0)),
            ],
        ),
        out_shape=[
            jax.ShapeDtypeStruct((batch, 2 * heads, half), jnp.float32),
            jax.ShapeDtypeStruct((batch, heads, lanes), jnp.float32),
        ],
        name="expand_gates",
    )(rel_len, cum_gates)


def attend_body(query_ref, cache_ref, bias_ref, last_ref, out_ref, *, scale):
    rows, length, width = cache_ref.shape
    heads = query_ref.shape[1] // 2
    half = length // 2
    size = width // 2

    def both(r):
        return jnp.concatenate([cache_ref[r, :half], cache_ref[r, half:]], axis=1)

    biased = [
        lax.dot_general(
            query_ref[r], both(r), (((1,), (1,)), ((), ())), preferred_element_type=jnp.float32
        )
        * scale
        - bias_ref[r]
        for r in range(rows)
    ]
    peaks = [jnp.max(x, axis=1, keepdims=True) for x in biased]
    peaks = [jnp.maximum(jnp.maximum(p[:heads], p[heads:]), masked_floor) for p in peaks]
    weights = [
        jnp.exp(x - jnp.concatenate([p, p], axis=0)) for x, p in zip(biased, peaks)
    ]
    totals = [jnp.sum(x, axis=1, keepdims=True) for x in weights]
    values = [
        jnp.dot(weights[r].astype(jnp.bfloat16), both(r), preferred_element_type=jnp.float32)
        for r in range(rows)
    ]
    lane = lax.broadcasted_iota(jnp.int32, (heads, width), 1)
    tiles = []
    for r in range(rows):
        tile = values[r][:heads, :width] + values[r][heads:, width:]
        total = totals[r][:heads] + totals[r][heads:]
        tile = jnp.where(lane == 0, peaks[r], jnp.where(lane == 1, total, tile))
        tiles.append(jnp.where(lane == 2, last_ref[r], tile))
    by_head = jnp.swapaxes(jnp.stack(tiles), 0, 1)
    lane = lax.broadcasted_iota(jnp.int32, (rows, width), 1)
    fields = [jnp.zeros((rows, width), jnp.float32) for _ in range(3)]
    for h in range(heads):
        tile = by_head[h]
        for f in range(3):
            fields[f] = jnp.where(lane == h, tile[:, f : f + 1], fields[f])
        if h % 2:
            pair = jnp.where(lane < size, pltpu.roll(by_head[h - 1], size, 1), tile)
            out_ref[:, (h - 1) * size : (h + 1) * size] = pair.astype(out_ref.dtype)
    stats = sum(write_field(fields[f], f, heads) for f in range(3))
    out_ref[:, heads * size :] = stats.astype(out_ref.dtype)


def attend(query, cache, bias, last, scale):
    batch, length, width = cache.shape
    rows = 8
    heads = query.shape[1] // 2

    def spec(*shape):
        return pl.BlockSpec((rows,) + shape, lambda i: (i, 0, 0))

    full = heads * width // 2 + lanes
    return pl.pallas_call(
        functools.partial(attend_body, scale=scale),
        grid=(batch // rows,),
        in_specs=[
            spec(2 * heads, 2 * width),
            spec(length, width),
            spec(2 * heads, length // 2),
            spec(heads, lanes),
        ],
        out_specs=pl.BlockSpec((rows, full), lambda i: (i, 0)),
        out_shape=jax.ShapeDtypeStruct((batch, full), jnp.bfloat16),
        name="attend",
    )(query, cache, bias, last)


def project_body(at_ref, tokens_ref, gain_ref, query_ref, key_ref, value_ref, gate_ref, out_ref):
    x = tokens_ref[...].astype(jnp.float32)
    squares = jnp.sum(x * x, axis=1, keepdims=True)
    normed = (x * gain_ref[...]).astype(jnp.bfloat16)
    start = 0
    for ref in (query_ref, key_ref, value_ref):
        part = jnp.dot(normed, ref[...], preferred_element_type=jnp.float32)
        out_ref[:, start : start + part.shape[1]] = part.astype(out_ref.dtype)
        start += part.shape[1]
    gate = lax.dot_general(
        normed, gate_ref[...], (((1,), (1,)), ((), ())), preferred_element_type=jnp.float32
    )
    rest = out_ref.shape[1] - start
    tail = jnp.concatenate(
        [gate, jnp.broadcast_to(squares, (x.shape[0], rest - gate.shape[1]))], axis=1
    )
    out_ref[:, start:] = tail.astype(out_ref.dtype)


def project(at, tokens, gain, w_query, w_key, w_value, gates):
    batch, cols = tokens.shape
    used = w_query.shape[1] + w_key.shape[1] + w_value.shape[1] + gates.shape[0] + 1
    total = used + -used % lanes

    def whole(x):
        return pl.BlockSpec(x.shape, lambda i, at: (0, 0))

    return pl.pallas_call(
        project_body,
        grid_spec=pltpu.PrefetchScalarGridSpec(
            num_scalar_prefetch=1,
            grid=(1,),
            in_specs=[whole(x) for x in (tokens, gain, w_query, w_key, w_value)]
            + [pl.BlockSpec((gates.shape[0], cols), lambda i, at: (0, at[0]))],
            out_specs=pl.BlockSpec((batch, total), lambda i, at: (0, 0)),
        ),
        out_shape=jax.ShapeDtypeStruct((batch, total), jnp.bfloat16),
        name="project",
    )(at, tokens, gain, w_query, w_key, w_value, gates)


def read_field(stats, index, heads):
    parts = [
        pltpu.roll(stats, (lanes - (3 * index + t) * heads) % lanes, 1) for t in range(3)
    ]
    return parts[0] + (parts[1] + parts[2])


def write_field(x, index, heads):
    high = rounded(x)
    mid = rounded(x - high)
    low = rounded(x - high - mid)
    out = 0.0
    for t, part in enumerate((high, mid, low)):
        out = out + pltpu.roll(part, (3 * index + t) * heads, 1)
    return out


def spread_factors(factors, heads, head_size):
    width = heads * head_size
    stacked = jnp.concatenate(factors, axis=0)
    high = rounded(stacked)
    pair = jnp.concatenate(
        [high.astype(jnp.bfloat16), (stacked - high).astype(jnp.bfloat16)], axis=1
    )
    spread = (
        lax.broadcasted_iota(jnp.int32, (2 * lanes, width), 1) // head_size
        == lax.broadcasted_iota(jnp.int32, (2 * lanes, width), 0) % lanes
    ).astype(jnp.bfloat16)
    wide = jnp.dot(pair, spread, preferred_element_type=jnp.float32)
    rows = factors[0].shape[0]
    return [wide[i * rows : (i + 1) * rows] for i in range(len(factors))]


def merge_stats(mine_ref, other_ref, heads, width):
    own_stats = mine_ref[:, width:].astype(jnp.float32)
    far_stats = other_ref[:, width:].astype(jnp.float32)
    used = lax.broadcasted_iota(jnp.int32, own_stats.shape, 1) < heads
    own_peak, far_peak = (read_field(s, 0, heads) for s in (own_stats, far_stats))
    own_sum, far_sum = (read_field(s, 1, heads) for s in (own_stats, far_stats))
    anchor = read_field(own_stats, 2, heads) + read_field(far_stats, 2, heads)
    own_peak, far_peak, anchor, own_sum, far_sum = (
        jnp.where(used, x, 0.0) for x in (own_peak, far_peak, anchor, own_sum, far_sum)
    )
    peak = jnp.maximum(own_peak, far_peak)
    own_factor = jnp.exp(own_peak - peak)
    far_factor = jnp.exp(far_peak - peak)
    total = own_sum * own_factor + far_sum * far_factor
    return used, peak, total, anchor, own_factor, far_factor


def merge_body(mine_ref, other_ref, out_ref, *, heads, head_size):
    width = heads * head_size
    used, peak, total, anchor, own_factor, far_factor = merge_stats(
        mine_ref, other_ref, heads, width
    )
    own_wide, far_wide = spread_factors(
        [jnp.where(used, own_factor, 0.0), jnp.where(used, far_factor, 0.0)], heads, head_size
    )
    values = own_wide * mine_ref[:, :width].astype(jnp.float32) + far_wide * other_ref[
        :, :width
    ].astype(jnp.float32)
    out_ref[:, :width] = values.astype(jnp.bfloat16)
    stats = (
        write_field(peak, 0, heads)
        + write_field(jnp.where(used, total, 0.0), 1, heads)
        + write_field(anchor, 2, heads)
    )
    out_ref[:, width:] = stats.astype(jnp.bfloat16)


def merge(mine, other, heads, head_size):
    return pl.pallas_call(
        functools.partial(merge_body, heads=heads, head_size=head_size),
        in_specs=[pl.BlockSpec(memory_space=pltpu.VMEM)] * 2,
        out_specs=pl.BlockSpec(memory_space=pltpu.VMEM),
        out_shape=jax.ShapeDtypeStruct(mine.shape, mine.dtype),
        name="merge",
    )(mine, other)


def finish_body(
    mine_ref, other_ref, fresh_ref, value_ref, attended_ref, log_ref, *, heads, head_size
):
    width = heads * head_size
    used, peak, total, anchor, own_factor, far_factor = merge_stats(
        mine_ref, other_ref, heads, width
    )
    fresh = fresh_ref[...]
    cum_query = anchor + pltpu.roll(fresh, lanes - heads, 1)
    fresh_biased = jnp.where(used, fresh - cum_query, 0.0)
    top = jnp.maximum(peak, fresh_biased)
    keep = jnp.exp(peak - top)
    fresh_weight = jnp.exp(fresh_biased - top)
    total = jnp.where(used, total * keep + fresh_weight, 1.0)
    factors = [own_factor * keep / total, far_factor * keep / total, rounded(fresh_weight) / total]
    own_wide, far_wide, fresh_wide = spread_factors(
        [jnp.where(used, f, 0.0) for f in factors], heads, head_size
    )
    values = (
        own_wide * mine_ref[:, :width].astype(jnp.float32)
        + far_wide * other_ref[:, :width].astype(jnp.float32)
        + fresh_wide * value_ref[...].astype(jnp.float32)
    )
    attended_ref[...] = values.astype(jnp.bfloat16)
    log_ref[...] = top + jnp.log(total) + cum_query


def finish(mine, other, fresh, value, heads, head_size):
    batch = mine.shape[0]
    return pl.pallas_call(
        functools.partial(finish_body, heads=heads, head_size=head_size),
        in_specs=[pl.BlockSpec(memory_space=pltpu.VMEM)] * 4,
        out_specs=[pl.BlockSpec(memory_space=pltpu.VMEM)] * 2,
        out_shape=[
            jax.ShapeDtypeStruct((batch, heads * head_size), jnp.bfloat16),
            jax.ShapeDtypeStruct((batch, lanes), jnp.float32),
        ],
        name="finish",
    )(mine, other, fresh, value)


def shards(
    tokens,
    norm_gain,
    w_query,
    w_key,
    w_value,
    forget_weight,
    forget_bias,
    kv_cache,
    cum_gates,
    lengths,
    w_out,
):
    batch, cols = tokens.shape
    span = kv_cache.shape[1]
    kv_local = kv_cache.shape[2]
    head_size = kv_cache.shape[3] // 2
    heads = cum_gates.shape[1]
    group = heads // kv_local
    width = heads * head_size
    kv_width = kv_local * head_size
    model_width = cols * lax.axis_size("kv")

    first_pos = lax.axis_index("kv") * span
    bias, last_cum = expand_gates(lengths - first_pos, cum_gates, kv_local, group)

    parts = project(
        lax.axis_index("kv").reshape(1),
        tokens,
        norm_gain.reshape(1, cols),
        w_query,
        w_key,
        w_value,
        forget_weight.T,
    )
    sums = exchange_sum(parts, "kv")

    edge = width + 2 * kv_width
    all_heads = forget_weight.shape[1]
    squares = sums[:, edge + all_heads : edge + all_heads + 1]
    row_scale = lax.rsqrt(squares / model_width + norm_eps)
    projected = (row_scale * sums[:, :edge]).astype(jnp.bfloat16)
    query = projected[:, :width]
    gates = lax.dynamic_slice(sums, (0, edge + lax.axis_index("tp") * heads), (batch, heads))
    log_gate = jax.nn.log_sigmoid(row_scale * gates + forget_bias)
    query_rows = query.reshape(batch, heads, head_size)
    full = 4 * head_size
    query_pair = jnp.concatenate(
        [
            jnp.pad(query_rows, ((0, 0), (0, 0), (0, full - head_size))),
            jnp.pad(query_rows, ((0, 0), (0, 0), (full // 2, full // 2 - head_size))),
        ],
        axis=1,
    )
    scale = head_size ** (-0.5)
    cache = kv_cache.reshape(batch, span * kv_local, 2 * head_size)
    packed = attend(query_pair, cache, bias, last_cum, scale)

    key_rows = projected[:, width : width + kv_width].reshape(batch, kv_local, 1, head_size)
    fresh_score = jnp.sum(
        query.reshape(batch, kv_local, group, head_size).astype(jnp.float32)
        * key_rows.astype(jnp.float32),
        axis=-1,
    ).reshape(batch, heads)
    fresh = jnp.concatenate(
        [
            fresh_score * scale,
            log_gate,
            jnp.zeros((batch, lanes - 2 * heads), jnp.float32),
        ],
        axis=1,
    )
    value_rows = projected[:, width + kv_width :].reshape(batch, kv_local, 1, head_size)
    value_wide = jnp.broadcast_to(value_rows, (batch, kv_local, group, head_size)).reshape(
        batch, width
    )

    step = 1
    while 2 * step < lax.axis_size("kv"):
        packed = merge(packed, xor_permute(packed, "kv", step), heads, head_size)
        step *= 2
    attended, log_weight = finish(
        packed, xor_permute(packed, "kv", step), fresh, value_wide, heads, head_size
    )
    part_out = jnp.dot(attended, w_out, preferred_element_type=jnp.float32)
    mixed = exchange_sum(part_out, "tp").astype(jnp.bfloat16)
    return (mixed, log_weight[:, :heads])


def solution(mesh):
    placed = (
        P(None, "kv"),
        P("kv"),
        P("kv", "tp"),
        P("kv", "tp"),
        P("kv", "tp"),
        P(),
        P("tp"),
        P(None, "kv", "tp", None),
        P(None, "tp", "kv"),
        P(),
        P("tp", "kv"),
    )
    return jax.shard_map(
        shards,
        mesh=mesh,
        in_specs=placed,
        out_specs=(P(None, "kv"), P(None, "tp")),
        check_vma=False,
    )
```

```python
import functools

import jax
import jax.numpy as jnp
from jax import lax
from jax.experimental import pallas as pl
from jax.experimental.pallas import tpu as pltpu
from jax.sharding import PartitionSpec as P

norm_eps = 1e-05
masked_floor = -1e30
lanes = 128


def in_vmem(x):
    return pltpu.with_memory_space_constraint(x, pltpu.VMEM)


def rounded(x):
    return x.astype(jnp.bfloat16).astype(jnp.float32)


def xor_permute(x, axis, step):
    size = lax.axis_size(axis)
    return lax.ppermute(x, axis, [(i, i ^ step) for i in range(size)])


def exchange_sum(x, axis):
    step = 1
    while step < lax.axis_size(axis):
        mine = lax.optimization_barrier(x.astype(jnp.bfloat16))
        other = xor_permute(mine, axis, step)
        x = mine.astype(jnp.float32) + other.astype(jnp.float32)
        step *= 2
    return x


def expand_body(lengths_ref, first_ref, cum_ref, bias_ref, last_ref, *, kv_local, group):
    rows, heads, span = cum_ref.shape
    wide = lanes * kv_local
    half = span * kv_local // 2
    spread = (
        lax.broadcasted_iota(jnp.int32, (lanes, wide), 1) // kv_local
        == lax.broadcasted_iota(jnp.int32, (lanes, wide), 0)
    ).astype(jnp.bfloat16)
    spread2 = jnp.concatenate([spread, spread], axis=0)
    col = lax.broadcasted_iota(jnp.int32, (heads, wide), 1)
    row_head = lax.broadcasted_iota(jnp.int32, (heads, wide), 0) // group
    own = col % kv_local == row_head
    local = col // kv_local
    narrow = lax.broadcasted_iota(jnp.int32, (heads, lanes), 1)
    base = pl.program_id(0) * rows
    rels = [lengths_ref[base + r] - first_ref[0] for r in range(rows)]
    last = [jnp.zeros((heads, lanes), jnp.float32) for _ in range(rows)]
    spread_rows = []
    for c in range(span // lanes):
        x = cum_ref[:, :, c * lanes : (c + 1) * lanes].reshape(rows * heads, lanes)
        high = rounded(x)
        mid = rounded(x - high)
        low = (x - high - mid).astype(jnp.bfloat16)
        pair = jnp.concatenate([high.astype(jnp.bfloat16), mid.astype(jnp.bfloat16)], axis=1)
        y = jnp.dot(pair, spread2, preferred_element_type=jnp.float32) + jnp.dot(
            low, spread, preferred_element_type=jnp.float32
        )
        spread_rows.append(y)
        for r in range(rows):
            last[r] = last[r] + jnp.where(
                narrow == rels[r] - 1 - c * lanes, x[r * heads : (r + 1) * heads], 0.0
            )
    for c in range(span // lanes):
        start = c * wide
        side = start // half
        start = start - side * half
        for r in range(rows):
            ok = own & (local < rels[r] - c * lanes)
            bias_ref[r, side * heads : (side + 1) * heads, start : start + wide] = jnp.where(
                ok, spread_rows[c][r * heads : (r + 1) * heads], -masked_floor
            )
    for r in range(rows):
        last_ref[r] = jnp.broadcast_to(jnp.sum(last[r], axis=1, keepdims=True), (heads, lanes))


def expand_gates(lengths, first_pos, cum_gates, kv_local, group):
    batch, heads, span = cum_gates.shape
    rows = 8
    half = span * kv_local // 2
    return pl.pallas_call(
        functools.partial(expand_body, kv_local=kv_local, group=group),
        grid_spec=pltpu.PrefetchScalarGridSpec(
            num_scalar_prefetch=2,
            grid=(batch // rows,),
            in_specs=[pl.BlockSpec((rows, heads, span), lambda i, n, f: (i, 0, 0))],
            out_specs=[
                pl.BlockSpec((rows, 2 * heads, half), lambda i, n, f: (i, 0, 0)),
                pl.BlockSpec((rows, heads, lanes), lambda i, n, f: (i, 0, 0)),
            ],
        ),
        out_shape=[
            jax.ShapeDtypeStruct((batch, 2 * heads, half), jnp.float32),
            jax.ShapeDtypeStruct((batch, heads, lanes), jnp.float32),
        ],
        name="expand_gates",
    )(lengths, first_pos, cum_gates)


def attend_body(query_ref, cache_ref, bias_ref, last_ref, out_ref, *, scale):
    rows, length, width = cache_ref.shape
    heads = query_ref.shape[1] // 2
    half = length // 2
    size = width // 2

    def both(r):
        return jnp.concatenate([cache_ref[r, :half], cache_ref[r, half:]], axis=1)

    biased = [
        lax.dot_general(
            query_ref[r], both(r), (((1,), (1,)), ((), ())), preferred_element_type=jnp.float32
        )
        * scale
        - bias_ref[r]
        for r in range(rows)
    ]
    peaks = [jnp.max(x, axis=1, keepdims=True) for x in biased]
    peaks = [jnp.maximum(jnp.maximum(p[:heads], p[heads:]), masked_floor) for p in peaks]
    weights = [
        jnp.exp(x - jnp.concatenate([p, p], axis=0)) for x, p in zip(biased, peaks)
    ]
    totals = [jnp.sum(x, axis=1, keepdims=True) for x in weights]
    values = [
        jnp.dot(weights[r].astype(jnp.bfloat16), both(r), preferred_element_type=jnp.float32)
        for r in range(rows)
    ]
    lane = lax.broadcasted_iota(jnp.int32, (heads, width), 1)
    tiles = []
    for r in range(rows):
        tile = values[r][:heads, :width] + values[r][heads:, width:]
        total = totals[r][:heads] + totals[r][heads:]
        tile = jnp.where(lane == 0, peaks[r], jnp.where(lane == 1, total, tile))
        tiles.append(jnp.where(lane == 2, last_ref[r], tile))
    by_head = jnp.swapaxes(jnp.stack(tiles), 0, 1)
    lane = lax.broadcasted_iota(jnp.int32, (rows, width), 1)
    fields = [jnp.zeros((rows, width), jnp.float32) for _ in range(3)]
    for h in range(heads):
        tile = by_head[h]
        for f in range(3):
            fields[f] = jnp.where(lane == h, tile[:, f : f + 1], fields[f])
        if h % 2:
            pair = jnp.where(lane < size, pltpu.roll(by_head[h - 1], size, 1), tile)
            out_ref[:, (h - 1) * size : (h + 1) * size] = pair.astype(out_ref.dtype)
    stats = sum(write_field(fields[f], f, heads) for f in range(3))
    out_ref[:, heads * size :] = stats.astype(out_ref.dtype)


def attend(query, cache, bias, last, scale):
    batch, length, width = cache.shape
    rows = 8
    heads = query.shape[1] // 2

    def spec(*shape):
        return pl.BlockSpec((rows,) + shape, lambda i: (i, 0, 0))

    full = heads * width // 2 + lanes
    return pl.pallas_call(
        functools.partial(attend_body, scale=scale),
        grid=(batch // rows,),
        in_specs=[
            spec(2 * heads, 2 * width),
            spec(length, width),
            spec(2 * heads, length // 2),
            spec(heads, lanes),
        ],
        out_specs=pl.BlockSpec((rows, full), lambda i: (i, 0)),
        out_shape=pltpu.VMEM((batch, full), jnp.bfloat16),
        name="attend",
    )(in_vmem(query), cache, bias, last)


def project_body(at_ref, tokens_ref, gain_ref, query_ref, key_ref, value_ref, gate_ref, out_ref):
    x = tokens_ref[...].astype(jnp.float32)
    squares = jnp.sum(x * x, axis=1, keepdims=True)
    normed = (x * gain_ref[...]).astype(jnp.bfloat16)
    start = 0
    for ref in (query_ref, key_ref, value_ref):
        part = jnp.dot(normed, ref[...], preferred_element_type=jnp.float32)
        out_ref[:, start : start + part.shape[1]] = part.astype(out_ref.dtype)
        start += part.shape[1]
    gate = lax.dot_general(
        normed, gate_ref[...], (((1,), (1,)), ((), ())), preferred_element_type=jnp.float32
    )
    rest = out_ref.shape[1] - start
    tail = jnp.concatenate(
        [gate, jnp.broadcast_to(squares, (x.shape[0], rest - gate.shape[1]))], axis=1
    )
    out_ref[:, start:] = tail.astype(out_ref.dtype)


def project(at, tokens, gain, w_query, w_key, w_value, gates):
    batch, cols = tokens.shape
    used = w_query.shape[1] + w_key.shape[1] + w_value.shape[1] + gates.shape[0] + 1
    total = used + -used % lanes

    def whole(x):
        return pl.BlockSpec(x.shape, lambda i, at: (0, 0))

    return pl.pallas_call(
        project_body,
        grid_spec=pltpu.PrefetchScalarGridSpec(
            num_scalar_prefetch=1,
            grid=(1,),
            in_specs=[whole(x) for x in (tokens, gain, w_query, w_key, w_value)]
            + [pl.BlockSpec((gates.shape[0], cols), lambda i, at: (0, at[0]))],
            out_specs=pl.BlockSpec((batch, total), lambda i, at: (0, 0)),
        ),
        out_shape=pltpu.VMEM((batch, total), jnp.bfloat16),
        name="project",
    )(at, tokens, gain, w_query, w_key, w_value, gates)


def read_field(stats, index, heads):
    parts = [
        pltpu.roll(stats, (lanes - (3 * index + t) * heads) % lanes, 1) for t in range(3)
    ]
    return parts[0] + (parts[1] + parts[2])


def write_field(x, index, heads):
    high = rounded(x)
    mid = rounded(x - high)
    low = rounded(x - high - mid)
    out = 0.0
    for t, part in enumerate((high, mid, low)):
        out = out + pltpu.roll(part, (3 * index + t) * heads, 1)
    return out


def spread_factors(factors, heads, head_size):
    width = heads * head_size
    stacked = jnp.concatenate(factors, axis=0)
    high = rounded(stacked)
    pair = jnp.concatenate(
        [high.astype(jnp.bfloat16), (stacked - high).astype(jnp.bfloat16)], axis=1
    )
    spread = (
        lax.broadcasted_iota(jnp.int32, (2 * lanes, width), 1) // head_size
        == lax.broadcasted_iota(jnp.int32, (2 * lanes, width), 0) % lanes
    ).astype(jnp.bfloat16)
    wide = jnp.dot(pair, spread, preferred_element_type=jnp.float32)
    rows = factors[0].shape[0]
    return [wide[i * rows : (i + 1) * rows] for i in range(len(factors))]


def merge_stats(mine_ref, other_ref, heads, width):
    own_stats = mine_ref[:, width:].astype(jnp.float32)
    far_stats = other_ref[:, width:].astype(jnp.float32)
    used = lax.broadcasted_iota(jnp.int32, own_stats.shape, 1) < heads
    own_peak, far_peak = (read_field(s, 0, heads) for s in (own_stats, far_stats))
    own_sum, far_sum = (read_field(s, 1, heads) for s in (own_stats, far_stats))
    anchor = read_field(own_stats, 2, heads) + read_field(far_stats, 2, heads)
    own_peak, far_peak, anchor, own_sum, far_sum = (
        jnp.where(used, x, 0.0) for x in (own_peak, far_peak, anchor, own_sum, far_sum)
    )
    peak = jnp.maximum(own_peak, far_peak)
    own_factor = jnp.exp(own_peak - peak)
    far_factor = jnp.exp(far_peak - peak)
    total = own_sum * own_factor + far_sum * far_factor
    return used, peak, total, anchor, own_factor, far_factor


def merge_body(mine_ref, other_ref, out_ref, *, heads, head_size):
    width = heads * head_size
    used, peak, total, anchor, own_factor, far_factor = merge_stats(
        mine_ref, other_ref, heads, width
    )
    own_wide, far_wide = spread_factors(
        [jnp.where(used, own_factor, 0.0), jnp.where(used, far_factor, 0.0)], heads, head_size
    )
    values = own_wide * mine_ref[:, :width].astype(jnp.float32) + far_wide * other_ref[
        :, :width
    ].astype(jnp.float32)
    out_ref[:, :width] = values.astype(jnp.bfloat16)
    stats = (
        write_field(peak, 0, heads)
        + write_field(jnp.where(used, total, 0.0), 1, heads)
        + write_field(anchor, 2, heads)
    )
    out_ref[:, width:] = stats.astype(jnp.bfloat16)


def merge(mine, other, heads, head_size):
    return pl.pallas_call(
        functools.partial(merge_body, heads=heads, head_size=head_size),
        in_specs=[pl.BlockSpec(memory_space=pltpu.VMEM)] * 2,
        out_specs=pl.BlockSpec(memory_space=pltpu.VMEM),
        out_shape=pltpu.VMEM(mine.shape, mine.dtype),
        name="merge",
    )(in_vmem(mine), in_vmem(other))


def finish_body(
    mine_ref, other_ref, fresh_ref, value_ref, attended_ref, log_ref, *, heads, head_size
):
    width = heads * head_size
    used, peak, total, anchor, own_factor, far_factor = merge_stats(
        mine_ref, other_ref, heads, width
    )
    fresh = fresh_ref[...]
    cum_query = anchor + pltpu.roll(fresh, lanes - heads, 1)
    fresh_biased = jnp.where(used, fresh - cum_query, 0.0)
    top = jnp.maximum(peak, fresh_biased)
    keep = jnp.exp(peak - top)
    fresh_weight = jnp.exp(fresh_biased - top)
    total = jnp.where(used, total * keep + fresh_weight, 1.0)
    factors = [own_factor * keep / total, far_factor * keep / total, rounded(fresh_weight) / total]
    own_wide, far_wide, fresh_wide = spread_factors(
        [jnp.where(used, f, 0.0) for f in factors], heads, head_size
    )
    values = (
        own_wide * mine_ref[:, :width].astype(jnp.float32)
        + far_wide * other_ref[:, :width].astype(jnp.float32)
        + fresh_wide * value_ref[...].astype(jnp.float32)
    )
    attended_ref[...] = values.astype(jnp.bfloat16)
    log_ref[...] = top + jnp.log(total) + cum_query


def finish(mine, other, fresh, value, heads, head_size):
    batch = mine.shape[0]
    return pl.pallas_call(
        functools.partial(finish_body, heads=heads, head_size=head_size),
        in_specs=[pl.BlockSpec(memory_space=pltpu.VMEM)] * 4,
        out_specs=[pl.BlockSpec(memory_space=pltpu.VMEM)] * 2,
        out_shape=[
            pltpu.VMEM((batch, heads * head_size), jnp.bfloat16),
            pltpu.VMEM((batch, lanes), jnp.float32),
        ],
        name="finish",
    )(in_vmem(mine), in_vmem(other), in_vmem(fresh), in_vmem(value))


def shards(
    tokens,
    norm_gain,
    w_query,
    w_key,
    w_value,
    forget_weight,
    forget_bias,
    kv_cache,
    cum_gates,
    lengths,
    w_out,
):
    batch, cols = tokens.shape
    span = kv_cache.shape[1]
    kv_local = kv_cache.shape[2]
    head_size = kv_cache.shape[3] // 2
    heads = cum_gates.shape[1]
    group = heads // kv_local
    width = heads * head_size
    kv_width = kv_local * head_size
    model_width = cols * lax.axis_size("kv")

    first_pos = lax.axis_index("kv") * span
    bias, last_cum = expand_gates(lengths, first_pos.reshape(1), cum_gates, kv_local, group)

    parts = project(
        lax.axis_index("kv").reshape(1),
        tokens,
        norm_gain.reshape(1, cols),
        w_query,
        w_key,
        w_value,
        forget_weight.T,
    )
    sums = exchange_sum(parts, "kv")

    edge = width + 2 * kv_width
    all_heads = forget_weight.shape[1]
    squares = sums[:, edge + all_heads : edge + all_heads + 1]
    row_scale = lax.rsqrt(squares / model_width + norm_eps)
    projected = (row_scale * sums[:, :edge]).astype(jnp.bfloat16)
    query = projected[:, :width]
    gates = lax.dynamic_slice(sums, (0, edge + lax.axis_index("tp") * heads), (batch, heads))
    log_gate = jax.nn.log_sigmoid(row_scale * gates + forget_bias)
    query_rows = query.reshape(batch, heads, head_size)
    full = 4 * head_size
    query_pair = jnp.concatenate(
        [
            jnp.pad(query_rows, ((0, 0), (0, 0), (0, full - head_size))),
            jnp.pad(query_rows, ((0, 0), (0, 0), (full // 2, full // 2 - head_size))),
        ],
        axis=1,
    )
    scale = head_size ** (-0.5)
    cache = kv_cache.reshape(batch, span * kv_local, 2 * head_size)
    packed = attend(query_pair, cache, bias, last_cum, scale)

    key_rows = projected[:, width : width + kv_width].reshape(batch, kv_local, 1, head_size)
    fresh_score = jnp.sum(
        query.reshape(batch, kv_local, group, head_size).astype(jnp.float32)
        * key_rows.astype(jnp.float32),
        axis=-1,
    ).reshape(batch, heads)
    fresh = jnp.concatenate(
        [
            fresh_score * scale,
            log_gate,
            jnp.zeros((batch, lanes - 2 * heads), jnp.float32),
        ],
        axis=1,
    )
    value_rows = projected[:, width + kv_width :].reshape(batch, kv_local, 1, head_size)
    value_wide = jnp.broadcast_to(value_rows, (batch, kv_local, group, head_size)).reshape(
        batch, width
    )

    step = 1
    while 2 * step < lax.axis_size("kv"):
        packed = merge(packed, xor_permute(packed, "kv", step), heads, head_size)
        step *= 2
    attended, log_weight = finish(
        packed, xor_permute(packed, "kv", step), fresh, value_wide, heads, head_size
    )
    part_out = jnp.dot(attended, w_out, preferred_element_type=jnp.float32)
    mixed = exchange_sum(part_out, "tp").astype(jnp.bfloat16)
    return (mixed, log_weight[:, :heads])


def solution(mesh):
    placed = (
        P(None, "kv"),
        P("kv"),
        P("kv", "tp"),
        P("kv", "tp"),
        P("kv", "tp"),
        P(),
        P("tp"),
        P(None, "kv", "tp", None),
        P(None, "tp", "kv"),
        P(),
        P("tp", "kv"),
    )
    return jax.shard_map(
        shards,
        mesh=mesh,
        in_specs=placed,
        out_specs=(P(None, "kv"), P(None, "tp")),
        check_vma=False,
    )
```
